32 devices in a mesh: grp: 2 (over y), ep: 4 (over z), tp: 4 (over x, core).
Axes of the slice: x: 2, y: 2, z: 4, core: 2. Of those that a mesh axis runs over, the one named last changes fastest.
Arguments:
- tokens: bfloat16 [2048, 2048], P(('grp', 'ep')), parts along dimension 0, may hold values from -6 to 6
- norm_gain: float32 [2048], replicated, may hold values from 0.1 to 1.9
- routing: int32 [2048, 2], P(('grp', 'ep')), parts along dimension 0, may hold values from 0 to 3, all different within a row; in each aligned block of 256 rows (0 to 255, 256 to 511, ...) at most 192 rows name the same one
- gate_weights: float32 [2048, 2], P(('grp', 'ep')), parts along dimension 0, may hold values from 0.2 to 2
- expert_gate: bfloat16 [4, 2048, 1024], P('ep', None, 'tp'), may hold values from -0.125 to 0.125
- expert_up: bfloat16 [4, 2048, 1024], P('ep', None, 'tp'), may hold values from -0.125 to 0.125
- expert_down: bfloat16 [4, 1024, 2048], P('ep', 'tp'), may hold values from -0.1875 to 0.1875
- shared_gate: bfloat16 [2048, 512], P(None, 'tp'), may hold values from -0.125 to 0.125
- shared_up: bfloat16 [2048, 512], P(None, 'tp'), may hold values from -0.125 to 0.125
- shared_down: bfloat16 [512, 2048], P('tp'), may hold values from -0.25 to 0.25
Outputs:
- mixed: bfloat16 [2048, 2048], P(('grp', 'ep'), 'tp'), parts along dimension 0
The draws below stay inside these ranges and needn't reach their ends.
There are 2 independent parts, one for each index of `grp`. The reference program is written for one: setup_inputs(seed, part) draws one part's arguments, and reference() takes and returns one part's arrays. A program takes and returns all parts, laid end to end along the dimension named above; an argument that names none is the same for every part. Nothing has to cross between parts.
Inputs may be any that keep to these rules, and one draw needn't show every extreme that they name: `routing`: each row names 2 different experts. Within each aligned block of 256 rows no expert is named by more than 192 rows, and in every draw some block has an expert named by exactly 192 rows.
All inputs are finite; a program needn't handle non-finite values.
Results may differ from the reference program's by a relative error of at most 0.012.
Values may be sent and summed in bfloat16 or wider, within the bound.
No kernel may reach another device: no remote copies, remote signals or barrier semaphores. Data moves between devices by JAX's collectives and lax.ppermute only.
A program may use at most 64 MiB of HBM per device.

```python
import math
import jax
import jax.numpy as jnp
import numpy as np
from jax import lax

D = 2048
FFE = 1024
FFS = 512
TOP_K = 2
TOK_DEV = 256
EXPERTS = 4
CAP = 192
TOKENS = 1024
N_EP = 4
N_TP = 4


def level_of(rng, extent, pieces, smallest, top_value):
    def one(axis_at, shards_of):
        heights = jax.random.uniform(jax.random.fold_in(jax.random.fold_in(rng, 6), axis_at), (shards_of,), jnp.float32, smallest / len(pieces), top_value / len(pieces))
        return jnp.repeat(jnp.exp(heights), extent[axis_at] // shards_of).reshape((-1,) + (1,) * (len(extent) - axis_at - 1))

    factor_of = one(*pieces[0])
    for cut in pieces[1:]:
        factor_of = factor_of * one(*cut)
    return factor_of


def routed_block(stream_key, own, number, rows, count, top, most, slope):
    ranking = jax.random.permutation(stream_key, count)
    heavy_load, ordinary = shares(count, rows * top, most, slope, True), shares(count, rows * top, most, slope, False)
    places = jnp.arange(count)

    def named(tallies, rotation):
        used = int((tallies > 0).sum())
        fixed = max(1, used // 4)
        shifted = fixed + (places - fixed + rotation * (used - fixed)) % max(1, count - fixed)
        return jnp.zeros((count,), jnp.int32).at[ranking[jnp.where(places < fixed, places, shifted)]].set(jnp.asarray(tallies, jnp.int32))

    tallies = jnp.where(number % 4 == 0, named(heavy_load, number // 4), named(ordinary, number - number // 4 - 1))
    mixed = jax.random.permutation(jax.random.fold_in(own, 3), count)
    giver, taker = mixed[0:count // 2 * 2:2], mixed[1:count // 2 * 2:2]
    room = jnp.minimum(tallies[giver] - 1, most - tallies[taker]) // 2
    room = jnp.where((giver == ranking[0]) | (taker == ranking[0]) | (tallies[taker] == 0), 0, jnp.maximum(room, 0))
    shifted = jax.random.randint(jax.random.fold_in(own, 4), (count // 2,), 0, 1 << 20) % (room + 1)
    tallies = tallies.at[giver].add(-shifted).at[taker].add(shifted)
    items = jnp.searchsorted(jnp.cumsum(tallies), jnp.arange(rows * top), side="right").astype(jnp.int32)
    grid = items.reshape(top, rows).T
    grid = grid[jax.random.permutation(jax.random.fold_in(own, 1), rows)]
    rotation = jax.random.randint(jax.random.fold_in(own, 2), (rows, 1), 0, top)
    return jnp.take_along_axis(grid, (jnp.arange(top)[None, :] + rotation) % top, axis=1)


def shares(number_of, total, limit, skew, full):
    portions = [(1 << 20) // math.isqrt(grade ** skew) + 1 for grade in range(1, number_of + 1)]
    largest = limit if full else min(limit, max(-(-total // number_of), total * portions[0] // sum(portions)))
    least = 1 if total - largest >= number_of - 1 else 0
    holding, rest = [largest] + [least] * (number_of - 1), total - largest - least * (number_of - 1)
    while rest > 0:
        free = [i for i in range(1, number_of) if holding[i] < largest] or [i for i in range(1, number_of) if holding[i] < limit]
        mass, remaining = sum([portions[i] for i in free]), rest
        for i in free:
            addition = min(limit - holding[i], max(1, remaining * portions[i] // mass), rest)
            holding[i] = holding[i] + addition
            rest = rest - addition
    return np.array(holding)


def bell_draw(own_key, dims, scale, reach, cuts=(), held_as=jnp.bfloat16):
    gain = level_of(own_key, dims, cuts, -0.22, 0.18) if cuts else 1.0
    result = jax.random.normal(own_key, dims, jnp.float32) * scale * gain
    return jnp.minimum(jnp.maximum(result, -reach), reach).astype(held_as)


def setup_inputs(seed: int = 0, part: int = 0) -> dict:
    streams_of = jax.random.split(jax.random.key(seed), 11)
    part_keys = jax.random.split(jax.random.fold_in(streams_of[10], part), 11)
    tokens = bell_draw(part_keys[0], (TOKENS, D), 1.0, 6.0, ((0, 4),))
    norm_gain = jnp.clip(1.0 + 0.18 * jax.random.normal(streams_of[1], (D,), jnp.float32), 0.1, 1.9)
    routing_keys = jax.random.split(jax.random.fold_in(part_keys[2], 1), TOKENS // TOK_DEV)
    routing_turns = jax.random.permutation(jax.random.fold_in(part_keys[2], 3), TOKENS // TOK_DEV)
    routing = jax.vmap(lambda own, number: routed_block(jax.random.fold_in(part_keys[2], 2), own, number, TOK_DEV, EXPERTS, TOP_K, CAP, 2))(routing_keys, routing_turns).reshape((TOKENS, TOP_K))
    gate_weights = jnp.clip(jnp.exp(math.log(2.0) - 2.3025851 * jax.random.uniform(part_keys[3], (TOKENS, TOP_K), jnp.float32) ** level_of(part_keys[3], (TOKENS, TOP_K), ((0, 4),), -0.2, 0.2)), 0.2, 2.0)
    expert_gate = bell_draw(streams_of[4], (EXPERTS, D, FFE), D ** -0.5, 0.125, ((0, 4), (2, 4)))
    expert_up = bell_draw(streams_of[5], (EXPERTS, D, FFE), D ** -0.5, 0.125, ((0, 4), (2, 4)))
    expert_down = bell_draw(streams_of[6], (EXPERTS, FFE, D), FFE ** -0.5, 0.1875, ((0, 4), (1, 4)))
    shared_gate = bell_draw(streams_of[7], (D, FFS), D ** -0.5, 0.125, ((1, 4),))
    shared_up = bell_draw(streams_of[8], (D, FFS), D ** -0.5, 0.125, ((1, 4),))
    shared_down = bell_draw(streams_of[9], (FFS, D), FFS ** -0.5, 0.25, ((0, 4),))
    return dict(tokens=tokens, norm_gain=norm_gain, routing=routing, gate_weights=gate_weights, expert_gate=expert_gate, expert_up=expert_up, expert_down=expert_down, shared_gate=shared_gate, shared_up=shared_up, shared_down=shared_down)


def norm_rows(tokens, norm_gain):
    values = tokens.astype(jnp.float32)
    scale = lax.rsqrt(lax.optimization_barrier(jnp.mean(values * values, axis=-1, keepdims=True)) + 1e-06)
    return (values * scale * norm_gain).astype(jnp.bfloat16)

def grouped_down(hidden, down):
    width = hidden.shape[1] // N_TP
    total = jnp.zeros((hidden.shape[0], down.shape[1]), jnp.float32)
    for group in range(N_TP):
        partial_sum = jnp.dot(hidden[:, group * width:(group + 1) * width], down[group * width:(group + 1) * width], preferred_element_type=jnp.float32)
        total = total + partial_sum.astype(jnp.bfloat16).astype(jnp.float32)
    return total

def swiglu_hidden(rows, w_gate, w_up):
    gate = jnp.dot(rows, w_gate, preferred_element_type=jnp.float32)
    up = jnp.dot(rows, w_up, preferred_element_type=jnp.float32)
    return (jax.nn.silu(gate) * up).astype(jnp.bfloat16)

def reference(tokens, norm_gain, routing, gate_weights, expert_gate, expert_up, expert_down, shared_gate, shared_up, shared_down):
    normed = norm_rows(tokens, norm_gain)
    assign = TOK_DEV * TOP_K
    blocks = routing.reshape(N_EP, assign).astype(jnp.int32)
    onehot = (blocks[:, :, None] == jnp.arange(EXPERTS, dtype=jnp.int32)[None, None, :]).astype(jnp.int32)
    slot = lax.optimization_barrier(jnp.sum(jnp.cumsum(onehot, axis=1) * onehot, axis=2)).astype(jnp.int32) - 1
    dest = blocks * CAP + slot
    owner = (jnp.arange(N_EP, dtype=jnp.int32)[:, None] * TOK_DEV + jnp.arange(assign, dtype=jnp.int32)[None, :] // TOP_K).astype(jnp.int32)

    def fill_table(where, who):
        return jnp.full((EXPERTS * CAP,), TOKENS, jnp.int32).at[where].set(who)
    table = jax.vmap(fill_table)(dest, owner)
    table = table.reshape(N_EP, EXPERTS, CAP).transpose(1, 0, 2).reshape(EXPERTS, N_EP * CAP)
    padded = jnp.concatenate([normed, jnp.zeros((1, D), jnp.bfloat16)], axis=0)

    def one_expert(items):
        index, w_gate, w_up, w_down = items
        hidden = swiglu_hidden(padded[index], w_gate, w_up)
        return grouped_down(hidden, w_down).astype(jnp.bfloat16)
    outputs = lax.map(one_expert, (table, expert_gate, expert_up, expert_down))
    flat_index = blocks * (N_EP * CAP) + jnp.arange(N_EP, dtype=jnp.int32)[:, None] * CAP + slot
    picked = outputs.reshape(EXPERTS * N_EP * CAP, D)[flat_index.reshape(TOKENS * TOP_K)]
    picked = picked.astype(jnp.float32).reshape(TOKENS, TOP_K, D)
    routed = lax.optimization_barrier(jnp.sum(picked * gate_weights[:, :, None], axis=1))
    shared_out = grouped_down(swiglu_hidden(normed, shared_gate, shared_up), shared_down)
    return (routed + shared_out).astype(jnp.bfloat16)
```

```python
import jax
import jax.numpy as jnp
from jax import lax
from jax.experimental import pallas as pl
from jax.experimental.pallas import tpu as pltpu
from jax.sharding import PartitionSpec as P

BF, F32 = jnp.bfloat16, jnp.float32
VM = pltpu.MemorySpace.VMEM
SM = pltpu.MemorySpace.SMEM


def norm_rows(tokens, norm_gain):
    values = tokens.astype(jnp.float32)
    scale = lax.rsqrt(jnp.mean(values * values, axis=-1, keepdims=True) + 1e-06)
    return (values * scale * norm_gain).astype(jnp.bfloat16)


def dot(a, b):
    return jnp.dot(a, b, preferred_element_type=F32)


def swiglu(gate, up):
    return (gate / (1.0 + jnp.exp(-gate)) * up).astype(BF)


def call(kernel, name, outs, args, scalars=1):
    n = len(args)
    return pl.pallas_call(
        kernel,
        name=name,
        out_shape=outs,
        in_specs=[pl.BlockSpec(memory_space=SM)] * scalars + [pl.BlockSpec(memory_space=VM)] * (n - scalars),
        out_specs=jax.tree.map(lambda _: pl.BlockSpec(memory_space=VM), outs),
        compiler_params=pltpu.CompilerParams(vmem_limit_bytes=48 * 1024 * 1024),
    )(*args)


def slots_of(routing, ep, experts, capacity):
    rows, top = routing.shape
    lanes = lax.broadcasted_iota(jnp.int32, (rows, 128), 1)
    hits = [(routing[:, k : k + 1] == lanes).astype(F32) for k in range(top)]
    named = sum(hits[1:], hits[0])
    at = lax.broadcasted_iota(jnp.int32, (rows, rows), 0)
    before = lax.broadcasted_iota(jnp.int32, (rows, rows), 1)
    lower = (before < at).astype(F32).astype(BF)
    earlier = dot(lower, named.astype(BF))
    places = []
    for k in range(top):
        slot = jnp.sum(earlier * hits[k], axis=1, keepdims=True)
        turn = routing[:, k : k + 1] - ep
        turn = jnp.where(turn < 0, turn + experts, turn)
        places.append((turn * capacity).astype(F32) + slot)
    return places


def fast_body(
    tokens, norm_gain, routing, gate_weights, expert_gate, expert_up, expert_down, shared_gate, shared_up, shared_down
):
    ep_count, tp_count = lax.axis_size("ep"), lax.axis_size("tp")
    rows, width = tokens.shape
    top = routing.shape[1]
    experts = ep_count
    capacity = max(2, 3 * rows * top // (2 * experts))
    quarter = width // tp_count
    hid = expert_gate.shape[2]
    shid = shared_gate.shape[1]
    ep, tp = lax.axis_index("ep"), lax.axis_index("tp")
    where = jnp.stack([ep, tp]).astype(jnp.int32)
    w_gate, w_up, w_down = expert_gate[0], expert_up[0], expert_down[0]
    shifts = list(range(1, ep_count))
    order = sorted(shifts, key=lambda s: (min(s, ep_count - s), s))

    def over_tp(x, m):
        return lax.ppermute(x, "tp", [(i, i ^ m) for i in range(tp_count)])

    def over_ep(x, s):
        return lax.ppermute(x, "ep", [(i, (i + s) % ep_count) for i in range(ep_count)])

    def dispatch(where_ref, tokens_ref, gain_ref, routing_ref, normed_ref, own_ref, *send_refs):
        ep_at, tp_at = where_ref[0], where_ref[1]
        values = tokens_ref[...].astype(F32)
        scale = lax.rsqrt(jnp.mean(values * values, axis=-1, keepdims=True) + 1e-06)
        normed_ref[...] = (values * scale * gain_ref[...]).astype(BF)
        places = slots_of(routing_ref[...], ep_at, experts, capacity)
        lanes = lax.broadcasted_iota(jnp.int32, (rows, 128), 1)
        packed = jnp.zeros((rows, 128), F32)
        for k in range(top):
            packed = jnp.where(lanes == k, places[k], packed)
        turned = packed.T
        col = turned[0:top, :].astype(jnp.int32)
        mine = normed_ref[:, pl.ds(pl.multiple_of(tp_at * quarter, quarter), quarter)]
        for s in [0] + order:
            index = lax.broadcasted_iota(jnp.int32, (capacity, rows), 0) + s * capacity
            pick = index == col[0:1, :]
            for k in range(1, top):
                pick = pick | (index == col[k : k + 1, :])
            pick = pick.astype(F32).astype(BF)
            if s == 0:
                own_ref[...] = dot(pick, normed_ref[...]).astype(BF)
            else:
                send_refs[order.index(s)][...] = dot(pick, mine).astype(BF)

    piece = jax.ShapeDtypeStruct((capacity, quarter), BF)
    normed, own, *sends = call(
        dispatch,
        "dispatch",
        [jax.ShapeDtypeStruct((rows, width), BF), jax.ShapeDtypeStruct((capacity, width), BF)] + [piece] * len(order),
        [where, tokens, norm_gain.reshape(1, width), routing],
    )
    arrived = [over_ep(x, s) for x, s in zip(sends, order)]

    def columns(m):
        return lax.dynamic_slice_in_dim(w_down, (tp ^ m) * quarter, quarter, 1)

    downs = [columns(0)] + [over_tp(columns(m), m) for m in range(1, tp_count)]

    def local(where_ref, normed_ref, own_ref, routing_ref, gw_ref, wg, wu, wd, sg, su, sd, *out_refs):
        ep_at, tp_at = where_ref[0], where_ref[1]
        hidden = swiglu(dot(own_ref[...], wg[...]), dot(own_ref[...], wu[...]))
        s_hidden = swiglu(dot(normed_ref[...], sg[...]), dot(normed_ref[...], su[...]))
        places = slots_of(routing_ref[...], ep_at, experts, capacity)
        lanes = lax.broadcasted_iota(jnp.int32, (rows, capacity), 1)
        picks = [(places[k].astype(jnp.int32) == lanes).astype(F32).astype(BF) for k in range(top)]
        pick = sum(picks[1:], picks[0])
        weight = jnp.zeros((rows, 1), F32)
        for k in range(top):
            here = places[k] < float(capacity)
            weight = weight + jnp.where(here, gw_ref[:, k : k + 1], 0.0)
        for m in range(tp_count):
            at = pl.ds(pl.multiple_of((tp_at ^ m) * quarter, quarter), quarter)
            term = dot(hidden, wd[:, at]).astype(BF)
            shared = dot(s_hidden, sd[:, at])
            out_refs[m][...] = (dot(pick, term) * weight + shared).astype(BF)

    out_piece = jax.ShapeDtypeStruct((rows, quarter), BF)
    partials = call(
        local,
        "local",
        [out_piece] * tp_count,
        [where, normed, own, routing, gate_weights, w_gate, w_up, w_down, shared_gate, shared_up, shared_down],
    )

    def first(where_ref, *refs):
        pieces, (wg, wu, out_ref) = refs[:tp_count], refs[tp_count:]
        tp_at = where_ref[1]
        gate = jnp.zeros((capacity, hid), F32)
        up = jnp.zeros((capacity, hid), F32)
        for m in range(tp_count):
            at = pl.ds(pl.multiple_of((tp_at ^ m) * quarter, quarter), quarter)
            gate = gate + dot(pieces[m][...], wg[at, :])
            up = up + dot(pieces[m][...], wu[at, :])
        out_ref[...] = swiglu(gate, up)

    def second(*refs):
        pieces, weights, out_ref = refs[:tp_count], refs[tp_count : 2 * tp_count], refs[-1]
        total = dot(pieces[0][...], weights[0][...])
        for m in range(1, tp_count):
            total = total + dot(pieces[m][...], weights[m][...])
        out_ref[...] = total.astype(BF)

    def gather_tp(x):
        have = {0: x}
        bit = tp_count // 2
        while bit:
            for m in sorted(have):
                have[m ^ bit] = over_tp(have[m], bit)
            bit //= 2
        return [have[m] for m in range(tp_count)]

    returned = []
    for x, s in zip(arrived, order):
        pieces = gather_tp(x)
        hidden = call(first, f"first{s}", jax.ShapeDtypeStruct((capacity, hid), BF), [where, *pieces, w_gate, w_up])
        hiddens = gather_tp(hidden)
        out = call(second, f"second{s}", piece, [*hiddens, *downs], scalars=0)
        returned.append(over_ep(out, ep_count - s))

    kept = [partials[0]] + [over_tp(partials[m], m) for m in range(1, tp_count)]

    def combine(where_ref, routing_ref, gw_ref, *refs):
        backs, parts, out_ref = refs[: len(order)], refs[len(order) : -1], refs[-1]
        places = slots_of(routing_ref[...], where_ref[0], experts, capacity)
        total = parts[0][...].astype(F32)
        for part in parts[1:]:
            total = total + part[...].astype(F32)
        lanes = lax.broadcasted_iota(jnp.int32, (rows, capacity), 1)
        for k in range(top):
            place = places[k].astype(jnp.int32)
            picked = jnp.zeros((rows, quarter), F32)
            for back, s in zip(backs, order):
                pick = (place == lanes + s * capacity).astype(F32).astype(BF)
                picked = picked + dot(pick, back[...])
            total = total + picked * gw_ref[:, k : k + 1]
        out_ref[...] = total.astype(BF)

    return call(combine, "combine", out_piece, [where, routing, gate_weights, *returned, *kept])


def general_body(
    tokens, norm_gain, routing, gate_weights, expert_gate, expert_up, expert_down, shared_gate, shared_up, shared_down
):
    ep_count = lax.axis_size("ep")
    tp_count = lax.axis_size("tp")
    tok_rows, width = tokens.shape
    top = routing.shape[1]
    local_experts = expert_gate.shape[0]
    experts = ep_count * local_experts
    capacity = max(2, 3 * tok_rows * top // (2 * experts))
    quarter = width // tp_count
    arrived_rows = ep_count * capacity
    normed = norm_rows(tokens, norm_gain)
    flat_experts = routing.reshape(-1)
    assign = flat_experts.shape[0]
    onehot = (flat_experts[:, None] == jnp.arange(experts, dtype=jnp.int32)[None, :]).astype(jnp.float32)
    lower = (jnp.arange(assign)[:, None] >= jnp.arange(assign)[None, :]).astype(jnp.float32)
    running = jnp.dot(lower, onehot, precision=lax.Precision.HIGHEST)
    slot = (jnp.sum(running * onehot, axis=1) - 1.0).astype(jnp.int32)
    dest = flat_experts * capacity + slot
    owner = jnp.arange(assign, dtype=jnp.int32) // top
    slot_token = jnp.full((experts * capacity,), tok_rows, jnp.int32).at[dest].set(owner)
    padded = jnp.concatenate([normed, jnp.zeros((1, width), jnp.bfloat16)], axis=0)
    outgoing = padded[slot_token].reshape(experts, capacity, width)
    position = lax.axis_index("tp")
    own_columns = lax.dynamic_slice_in_dim(outgoing, position * quarter, quarter, 2)
    arrived = lax.all_to_all(own_columns, "ep", split_axis=0, concat_axis=0, tiled=True)
    piece = lax.all_gather(arrived, "tp", axis=2, tiled=True)
    piece = piece.reshape(ep_count, local_experts, capacity, width)
    routed_list = []
    for local in range(local_experts):
        rows = piece[:, local].reshape(arrived_rows, width)
        gate = jnp.dot(rows, expert_gate[local], preferred_element_type=jnp.float32)
        up = jnp.dot(rows, expert_up[local], preferred_element_type=jnp.float32)
        hidden = (jax.nn.silu(gate) * up).astype(jnp.bfloat16)
        term = jnp.dot(hidden, expert_down[local], preferred_element_type=jnp.float32)
        routed_list.append(term.reshape(ep_count, capacity, width))
    routed_terms = jnp.stack(routed_list, axis=1).reshape(experts * capacity, width)
    shared_gate_rows = jnp.dot(normed, shared_gate, preferred_element_type=jnp.float32)
    shared_up_rows = jnp.dot(normed, shared_up, preferred_element_type=jnp.float32)
    shared_hidden = (jax.nn.silu(shared_gate_rows) * shared_up_rows).astype(jnp.bfloat16)
    shared_term = jnp.dot(shared_hidden, shared_down, preferred_element_type=jnp.float32)
    routed_sum, shared_sum = (
        lax.psum_scatter(x.astype(jnp.bfloat16), "tp", scatter_dimension=1, tiled=True).astype(jnp.float32)
        for x in (routed_terms, shared_term)
    )
    expert_out = routed_sum.astype(jnp.bfloat16).reshape(experts, capacity, quarter)
    returned = lax.all_to_all(expert_out, "ep", split_axis=0, concat_axis=0, tiled=True)
    picked = returned.reshape(experts * capacity, quarter)[dest]
    picked = picked.astype(jnp.float32).reshape(tok_rows, top, quarter)
    routed = jnp.sum(picked * gate_weights[:, :, None], axis=1)
    return (routed + shared_sum).astype(jnp.bfloat16)


def solution(mesh):
    in_specs = (
        P(("grp", "ep"), None),
        P(),
        P(("grp", "ep"), None),
        P(("grp", "ep"), None),
        P("ep", None, "tp"),
        P("ep", None, "tp"),
        P("ep", "tp", None),
        P(None, "tp"),
        P(None, "tp"),
        P("tp", None),
    )
    ep_count, tp_count = mesh.shape["ep"], mesh.shape["tp"]

    def step(*args):
        short = ep_count <= 8 and tp_count & (tp_count - 1) == 0 and args[4].shape[0] == ep_count
        body = fast_body if short else general_body
        return jax.shard_map(
            body, mesh=mesh, in_specs=in_specs, out_specs=P(("grp", "ep"), "tp"), check_vma=False
        )(*args)

    return step
```

```python
import jax
import jax.numpy as jnp
from jax import lax
from jax.experimental import pallas as pl
from jax.experimental.pallas import tpu as pltpu
from jax.sharding import PartitionSpec as P


VMEM_MIB = 12
BF, F32 = jnp.bfloat16, jnp.float32
VM = pltpu.MemorySpace.VMEM
SM = pltpu.MemorySpace.SMEM


def norm_rows(tokens, norm_gain):
    values = tokens.astype(jnp.float32)
    scale = lax.rsqrt(jnp.mean(values * values, axis=-1, keepdims=True) + 1e-06)
    return (values * scale * norm_gain).astype(jnp.bfloat16)


def dot(a, b):
    return jnp.dot(a, b, preferred_element_type=F32)


def swiglu(gate, up):
    return (gate / (1.0 + jnp.exp(-gate)) * up).astype(BF)


def call(kernel, outs, args, scalars=1):
    n = len(args)
    return pl.pallas_call(
        kernel,
        out_shape=outs,
        in_specs=[pl.BlockSpec(memory_space=SM)] * scalars + [pl.BlockSpec(memory_space=VM)] * (n - scalars),
        out_specs=jax.tree.map(lambda _: pl.BlockSpec(memory_space=VM), outs),
        compiler_params=pltpu.CompilerParams(vmem_limit_bytes=VMEM_MIB * 1024 * 1024),
    )(*args)


def slots_of(routing, ep, experts, capacity):
    rows, top = routing.shape
    lanes = lax.broadcasted_iota(jnp.int32, (rows, 128), 1)
    hits = [(routing[:, k : k + 1] == lanes).astype(F32) for k in range(top)]
    named = sum(hits[1:], hits[0])
    at = lax.broadcasted_iota(jnp.int32, (rows, rows), 0)
    before = lax.broadcasted_iota(jnp.int32, (rows, rows), 1)
    lower = (before < at).astype(F32).astype(BF)
    earlier = dot(lower, named.astype(BF))
    places = []
    for k in range(top):
        slot = jnp.sum(earlier * hits[k], axis=1, keepdims=True)
        turn = routing[:, k : k + 1] - ep
        turn = jnp.where(turn < 0, turn + experts, turn)
        places.append((turn * capacity).astype(F32) + slot)
    return places


def fast_body(
    tokens, norm_gain, routing, gate_weights, expert_gate, expert_up, expert_down, shared_gate, shared_up, shared_down
):
    ep_count, tp_count = lax.axis_size("ep"), lax.axis_size("tp")
    rows, width = tokens.shape
    top = routing.shape[1]
    experts = ep_count
    capacity = max(2, 3 * rows * top // (2 * experts))
    quarter = width // tp_count
    hid = expert_gate.shape[2]
    ep, tp = lax.axis_index("ep"), lax.axis_index("tp")
    where = jnp.stack([ep, tp]).astype(jnp.int32)
    w_gate, w_up, w_down = expert_gate[0], expert_up[0], expert_down[0]
    order = shift_order(ep_count)
    lows = [1 << i for i in range(tp_count.bit_length() - 1)]
    highs = lows[::-1]

    def over_tp(x, m):
        return lax.ppermute(x, "tp", [(i, i ^ m) for i in range(tp_count)])

    def over_ep(x, s):
        return lax.ppermute(x, "ep", [(i, (i + s) % ep_count) for i in range(ep_count)])

    def at_quarter(tp_at, m):
        return pl.ds(pl.multiple_of((tp_at ^ m) * quarter, quarter), quarter)

    def cut(where_ref, down_ref, *refs):
        out_refs, sems = refs[:tp_count], refs[tp_count]
        tp_at = where_ref[1]
        copies = [
            pltpu.make_async_copy(down_ref.at[:, at_quarter(tp_at, m)], out_refs[m], sems.at[m]) for m in range(tp_count)
        ]
        for c in copies:
            c.start()
        for c in copies:
            c.wait()

    columns = pl.pallas_call(
        cut,
        name="cut",
        out_shape=[jax.ShapeDtypeStruct((hid, quarter), BF)] * tp_count,
        in_specs=[pl.BlockSpec(memory_space=SM), pl.BlockSpec(memory_space=pl.ANY)],
        out_specs=[pl.BlockSpec(memory_space=VM)] * tp_count,
        scratch_shapes=[pltpu.SemaphoreType.DMA((tp_count,))],
    )(where, w_down)
    downs = [columns[0]] + [over_tp(columns[m], m) for m in range(1, tp_count)]

    def dispatch(where_ref, tokens_ref, gain_ref, routing_ref, normed_ref, own_ref, *send_refs):
        ep_at, tp_at = where_ref[0], where_ref[1]
        values = tokens_ref[...].astype(F32)
        scale = lax.rsqrt(jnp.mean(values * values, axis=-1, keepdims=True) + 1e-06)
        normed_ref[...] = (values * scale * gain_ref[...]).astype(BF)
        places = slots_of(routing_ref[...], ep_at, experts, capacity)
        lanes = lax.broadcasted_iota(jnp.int32, (rows, 128), 1)
        packed = jnp.zeros((rows, 128), F32)
        for k in range(top):
            packed = jnp.where(lanes == k, places[k], packed)
        turned = packed.T
        col = turned[0:top, :].astype(jnp.int32)
        mine = normed_ref[:, at_quarter(tp_at, 0)]
        for s in order + [0]:
            index = lax.broadcasted_iota(jnp.int32, (capacity, rows), 0) + s * capacity
            pick = index == col[0:1, :]
            for k in range(1, top):
                pick = pick | (index == col[k : k + 1, :])
            pick = pick.astype(F32).astype(BF)
            if s == 0:
                own_ref[...] = dot(pick, normed_ref[...]).astype(BF)
            else:
                send_refs[order.index(s)][...] = dot(pick, mine).astype(BF)

    piece = jax.ShapeDtypeStruct((capacity, quarter), BF)
    normed, own, *sends = call(
        dispatch,
        [jax.ShapeDtypeStruct((rows, width), BF), jax.ShapeDtypeStruct((capacity, width), BF)] + [piece] * len(order),
        [where, tokens, norm_gain.reshape(1, width), routing],
    )
    arrived = [over_ep(x, s) for x, s in zip(sends, order)]

    def local(where_ref, normed_ref, own_ref, routing_ref, gw_ref, wg, wu, wd, sg, su, sd, *out_refs):
        ep_at, tp_at = where_ref[0], where_ref[1]
        hidden = swiglu(dot(own_ref[...], wg[...]), dot(own_ref[...], wu[...]))
        s_hidden = swiglu(dot(normed_ref[...], sg[...]), dot(normed_ref[...], su[...]))
        places = slots_of(routing_ref[...], ep_at, experts, capacity)
        lanes = lax.broadcasted_iota(jnp.int32, (rows, capacity), 1)
        picks = [(places[k].astype(jnp.int32) == lanes).astype(F32).astype(BF) for k in range(top)]
        pick = sum(picks[1:], picks[0])
        weight = jnp.zeros((rows, 1), F32)
        for k in range(top):
            here = places[k] < float(capacity)
            weight = weight + jnp.where(here, gw_ref[:, k : k + 1], 0.0)
        for m in range(tp_count):
            at = at_quarter(tp_at, m)
            term = dot(hidden, wd[:, at]).astype(BF)
            shared = dot(s_hidden, sd[:, at])
            out_refs[m][...] = (dot(pick, term) * weight + shared).astype(BF)

    out_piece = jax.ShapeDtypeStruct((rows, quarter), BF)
    partials = call(
        local,
        [out_piece] * tp_count,
        [where, normed, own, routing, gate_weights, w_gate, w_up, w_down, shared_gate, shared_up, shared_down],
    )

    def add(*refs):
        n = len(refs) // 3
        for i in range(n):
            refs[2 * n + i][...] = (refs[i][...].astype(F32) + refs[n + i][...].astype(F32)).astype(BF)

    parts = dict(enumerate(partials))
    for bit in lows[:-1]:
        keep = [m for m in sorted(parts) if not m & bit]
        came = [over_tp(parts[m ^ bit], bit) for m in keep]
        sums = call(add, [out_piece] * len(keep), [parts[m] for m in keep] + came, scalars=0)
        parts = dict(zip(keep, sums))
    bit = lows[-1]
    kept = [parts[0], over_tp(parts[bit], bit)]

    def first(where_ref, *refs):
        pieces, (wg, wu, out_ref) = refs[:tp_count], refs[tp_count:]
        tp_at = where_ref[1]
        gate = jnp.zeros((capacity, hid), F32)
        up = jnp.zeros((capacity, hid), F32)
        for m in range(tp_count):
            at = at_quarter(tp_at, m)
            gate = gate + dot(pieces[m][...], wg[at, :])
            up = up + dot(pieces[m][...], wu[at, :])
        out_ref[...] = swiglu(gate, up)

    def second(*refs):
        pieces, weights, out_ref = refs[:tp_count], refs[tp_count : 2 * tp_count], refs[-1]
        total = dot(pieces[0][...], weights[0][...])
        for m in range(1, tp_count):
            total = total + dot(pieces[m][...], weights[m][...])
        out_ref[...] = total.astype(BF)

    def gather_tp(x):
        have = {0: x}
        for bit in highs:
            for m in sorted(have):
                have[m ^ bit] = over_tp(have[m], bit)
        return [have[m] for m in range(tp_count)]

    def choose(where_ref, routing_ref, *pick_refs):
        places = slots_of(routing_ref[...], where_ref[0], experts, capacity)
        lanes = lax.broadcasted_iota(jnp.int32, (rows, capacity), 1)
        for i, s in enumerate(order):
            for k in range(top):
                place = places[k].astype(jnp.int32)
                pick_refs[i * top + k][...] = (place == lanes + s * capacity).astype(F32).astype(BF)

    picks = call(choose, [jax.ShapeDtypeStruct((rows, capacity), BF)] * (top * len(order)), [where, routing])

    returned = []
    for x, s in zip(arrived, order):
        pieces = gather_tp(x)
        hidden = call(first, jax.ShapeDtypeStruct((capacity, hid), BF), [where, *pieces, w_gate, w_up])
        hiddens = gather_tp(hidden)
        out = call(second, piece, [*hiddens, *downs], scalars=0)
        returned.append(over_ep(out, ep_count - s))

    def combine(gw_ref, *refs):
        starts, chosen, back, out_ref = refs[: -top - 2], refs[-top - 2 : -2], refs[-2], refs[-1]
        total = starts[0][...].astype(F32)
        for part in starts[1:]:
            total = total + part[...].astype(F32)
        for k in range(top):
            total = total + dot(chosen[k][...], back[...]) * gw_ref[:, k : k + 1]
        out_ref[...] = total.astype(out_ref.dtype)

    total = kept
    for i, (back, s) in enumerate(zip(returned, order)):
        kind = out_piece if i + 1 == len(order) else jax.ShapeDtypeStruct((rows, quarter), F32)
        total = [call(combine, kind, [gate_weights, *total, *picks[i * top : i * top + top], back], scalars=0)]
    return total[0]


def shift_order(ep_count):
    return sorted(range(1, ep_count), key=lambda s: (min(s, ep_count - s), s))


def general_body(
    tokens, norm_gain, routing, gate_weights, expert_gate, expert_up, expert_down, shared_gate, shared_up, shared_down
):
    ep_count = lax.axis_size("ep")
    tp_count = lax.axis_size("tp")
    tok_rows, width = tokens.shape
    top = routing.shape[1]
    local_experts = expert_gate.shape[0]
    experts = ep_count * local_experts
    capacity = max(2, 3 * tok_rows * top // (2 * experts))
    quarter = width // tp_count
    arrived_rows = ep_count * capacity
    normed = norm_rows(tokens, norm_gain)
    flat_experts = routing.reshape(-1)
    assign = flat_experts.shape[0]
    onehot = (flat_experts[:, None] == jnp.arange(experts, dtype=jnp.int32)[None, :]).astype(jnp.float32)
    lower = (jnp.arange(assign)[:, None] >= jnp.arange(assign)[None, :]).astype(jnp.float32)
    running = jnp.dot(lower, onehot, precision=lax.Precision.HIGHEST)
    slot = (jnp.sum(running * onehot, axis=1) - 1.0).astype(jnp.int32)
    dest = flat_experts * capacity + slot
    owner = jnp.arange(assign, dtype=jnp.int32) // top
    slot_token = jnp.full((experts * capacity,), tok_rows, jnp.int32).at[dest].set(owner)
    padded = jnp.concatenate([normed, jnp.zeros((1, width), jnp.bfloat16)], axis=0)
    outgoing = padded[slot_token].reshape(experts, capacity, width)
    position = lax.axis_index("tp")
    own_columns = lax.dynamic_slice_in_dim(outgoing, position * quarter, quarter, 2)
    arrived = lax.all_to_all(own_columns, "ep", split_axis=0, concat_axis=0, tiled=True)
    piece = lax.all_gather(arrived, "tp", axis=2, tiled=True)
    piece = piece.reshape(ep_count, local_experts, capacity, width)
    routed_list = []
    for local in range(local_experts):
        rows = piece[:, local].reshape(arrived_rows, width)
        gate = jnp.dot(rows, expert_gate[local], preferred_element_type=jnp.float32)
        up = jnp.dot(rows, expert_up[local], preferred_element_type=jnp.float32)
        hidden = (jax.nn.silu(gate) * up).astype(jnp.bfloat16)
        term = jnp.dot(hidden, expert_down[local], preferred_element_type=jnp.float32)
        routed_list.append(term.reshape(ep_count, capacity, width))
    routed_terms = jnp.stack(routed_list, axis=1).reshape(experts * capacity, width)
    shared_gate_rows = jnp.dot(normed, shared_gate, preferred_element_type=jnp.float32)
    shared_up_rows = jnp.dot(normed, shared_up, preferred_element_type=jnp.float32)
    shared_hidden = (jax.nn.silu(shared_gate_rows) * shared_up_rows).astype(jnp.bfloat16)
    shared_term = jnp.dot(shared_hidden, shared_down, preferred_element_type=jnp.float32)
    routed_sum, shared_sum = (
        lax.psum_scatter(x.astype(jnp.bfloat16), "tp", scatter_dimension=1, tiled=True).astype(jnp.float32)
        for x in (routed_terms, shared_term)
    )
    expert_out = routed_sum.astype(jnp.bfloat16).reshape(experts, capacity, quarter)
    returned = lax.all_to_all(expert_out, "ep", split_axis=0, concat_axis=0, tiled=True)
    picked = returned.reshape(experts * capacity, quarter)[dest]
    picked = picked.astype(jnp.float32).reshape(tok_rows, top, quarter)
    routed = jnp.sum(picked * gate_weights[:, :, None], axis=1)
    return (routed + shared_sum).astype(jnp.bfloat16)


def solution(mesh):
    in_specs = (
        P(("grp", "ep"), None),
        P(),
        P(("grp", "ep"), None),
        P(("grp", "ep"), None),
        P("ep", None, "tp"),
        P("ep", None, "tp"),
        P("ep", "tp", None),
        P(None, "tp"),
        P(None, "tp"),
        P("tp", None),
    )
    ep_count, tp_count = mesh.shape["ep"], mesh.shape["tp"]
    short = 4 == ep_count and tp_count == 4

    def step(body):
        return jax.shard_map(body, mesh=mesh, in_specs=in_specs, out_specs=P(("grp", "ep"), "tp"), check_vma=False)

    if short:
        return step(fast_body)
    return step(general_body)
```

```python
import jax
import jax.numpy as jnp
from jax import lax
from jax.experimental import pallas as pl
from jax.experimental.pallas import tpu as pltpu
from jax.sharding import PartitionSpec as P


BF, F32 = jnp.bfloat16, jnp.float32
VM = pltpu.MemorySpace.VMEM


def norm_rows(tokens, norm_gain):
    values = tokens.astype(jnp.float32)
    scale = lax.rsqrt(jnp.mean(values * values, axis=-1, keepdims=True) + 1e-06)
    return (values * scale * norm_gain).astype(jnp.bfloat16)


def dot(a, b):
    return jnp.dot(a, b, preferred_element_type=F32)


def swiglu(gate, up):
    return (gate / (1.0 + jnp.exp(-gate)) * up).astype(BF)


def call(kernel, outs, args, mib=16, **more):
    return pl.pallas_call(
        kernel,
        out_shape=outs,
        in_specs=[pl.BlockSpec(memory_space=VM)] * len(args),
        out_specs=jax.tree.map(lambda _: pl.BlockSpec(memory_space=VM), outs),
        compiler_params=pltpu.CompilerParams(vmem_limit_bytes=mib * 1024 * 1024),
        **more,
    )(*args)


def places_of(routing, ep, experts, capacity):
    top, rows = routing.shape
    expert = lax.broadcasted_iota(jnp.int32, (max(8, experts), rows), 0)
    hits = [(routing[k : k + 1, :] == expert).astype(F32) for k in range(top)]
    named = sum(hits[1:], hits[0])
    before = lax.broadcasted_iota(jnp.int32, (rows, rows), 0)
    at = lax.broadcasted_iota(jnp.int32, (rows, rows), 1)
    earlier = dot(named.astype(BF), (before < at).astype(F32).astype(BF))
    places = []
    for k in range(top):
        slot = jnp.sum(earlier * hits[k], axis=0, keepdims=True)
        turn = routing[k : k + 1, :] - ep
        turn = jnp.where(turn < 0, turn + experts, turn)
        places.append((turn * capacity).astype(F32) + slot)
    return places


def fast_body(
    tokens, norm_gain, routing, gate_weights, expert_gate, expert_up, expert_down, shared_gate, shared_up, shared_down
):
    ep_count, tp_count = lax.axis_size("ep"), lax.axis_size("tp")
    rows, width = tokens.shape
    top = routing.shape[1]
    experts = ep_count
    capacity = max(2, 3 * rows * top // (2 * experts))
    quarter = width // tp_count
    half = width // 2
    part = capacity // CORES
    w_gate, w_up, w_down = expert_gate[0], expert_up[0], expert_down[0]
    order = shift_order(ep_count)
    routing, gate_weights = routing.T, gate_weights.T

    def over_tp(x, m):
        return lax.ppermute(x, "tp", [(i, i ^ m) for i in range(tp_count)])

    def over_ep(x, s):
        return lax.ppermute(x, "ep", [(i, (i + s) % ep_count) for i in range(ep_count)])

    def at_quarter(m):
        return pl.ds(pl.multiple_of((lax.axis_index("tp") ^ m) * quarter, quarter), quarter)

    def at_half(other):
        chip = lax.axis_index("tp") // CORES
        return pl.ds(pl.multiple_of((1 - chip if other else chip) * half, half), half)

    near_gate, near_up = over_tp(w_gate, 1), over_tp(w_up, 1)
    near_down = over_tp(w_down, 1)

    def dispatch(tokens_ref, gain_ref, routing_ref, normed_ref, *send_refs):
        values = tokens_ref[...].astype(F32)
        scale = lax.rsqrt(jnp.mean(values * values, axis=-1, keepdims=True) + 1e-06)
        normed_ref[...] = (values * scale * gain_ref[...]).astype(BF)
        places = places_of(routing_ref[...], lax.axis_index("ep"), experts, capacity)
        places = [p.astype(jnp.int32) for p in places]
        mine = normed_ref[:, at_half(False)]
        base = (lax.axis_index("tp") % CORES) * part
        for send_ref, s in zip(send_refs, order):
            index = lax.broadcasted_iota(jnp.int32, (part, rows), 0) + (base + s * capacity)
            pick = (index == places[0]).astype(F32)
            for p in places[1:]:
                pick = pick + (index == p).astype(F32)
            send_ref[...] = dot(pick.astype(BF), mine).astype(BF)

    piece = jax.ShapeDtypeStruct((part, half), BF)
    normed, *sends = call(
        dispatch,
        [jax.ShapeDtypeStruct((rows, width), BF)] + [piece] * len(order),
        [tokens, norm_gain.reshape(1, width), routing],
    )
    arrived = [over_ep(x, s) for x, s in zip(sends, order)]

    def local(normed_ref, routing_ref, gw_ref, wg, wu, wd, sg, su, sd, *refs):
        out_refs, info_ref, pick_refs = refs[:tp_count], refs[tp_count], refs[tp_count + 1 :]
        places = places_of(routing_ref[...], lax.axis_index("ep"), experts, capacity)
        index = lax.broadcasted_iota(jnp.int32, (capacity, rows), 0)
        own = (index == places[0].astype(jnp.int32)).astype(F32)
        for p in places[1:]:
            own = own + (index == p.astype(jnp.int32)).astype(F32)
        own_rows = dot(own.astype(BF), normed_ref[...]).astype(BF)
        hidden = swiglu(dot(own_rows, wg[...]), dot(own_rows, wu[...]))
        s_hidden = swiglu(dot(normed_ref[...], sg[...]), dot(normed_ref[...], su[...]))
        info = jnp.zeros((128, rows), F32)
        line = lax.broadcasted_iota(jnp.int32, (128, rows), 0)
        for k in range(top):
            info = jnp.where(line == k, places[k], info)
            info = jnp.where(line == top + k, gw_ref[k : k + 1, :], info)
        info = info.T
        info_ref[...] = info
        lanes = lax.broadcasted_iota(jnp.int32, (rows, capacity), 1)
        columns = [info[:, k : k + 1].astype(jnp.int32) for k in range(top)]
        weights = [info[:, top + k : top + k + 1] for k in range(top)]
        pick = (columns[0] == lanes).astype(F32)
        weight = jnp.where(columns[0] < capacity, weights[0], 0.0)
        for k in range(1, top):
            pick = pick + (columns[k] == lanes).astype(F32)
            weight = weight + jnp.where(columns[k] < capacity, weights[k], 0.0)
        pick = pick.astype(BF)
        for m in range(tp_count):
            term = dot(hidden, wd[:, at_quarter(m)]).astype(BF)
            shared = dot(s_hidden, sd[:, at_quarter(m)])
            out_refs[m][...] = (dot(pick, term) * weight + shared).astype(BF)
        lanes = lax.broadcasted_iota(jnp.int32, (rows, part), 1)
        base = (lax.axis_index("tp") % CORES) * part
        for i, s in enumerate(order):
            for k in range(top):
                pick_refs[i * top + k][...] = (columns[k] == lanes + (base + s * capacity)).astype(F32).astype(BF)

    out_piece = jax.ShapeDtypeStruct((rows, quarter), BF)
    partials = call(
        local,
        [out_piece] * tp_count
        + [jax.ShapeDtypeStruct((rows, 128), F32)]
        + [jax.ShapeDtypeStruct((rows, part), BF)] * (top * len(order)),
        [normed, routing, gate_weights, w_gate, w_up, w_down, shared_gate, shared_up, shared_down],
    )
    info, picks = partials[tp_count], partials[tp_count + 1 :]
    partials = partials[:tp_count]

    def add(*refs):
        n = len(refs) // 3
        for i in range(n):
            refs[2 * n + i][...] = (refs[i][...].astype(F32) + refs[n + i][...].astype(F32)).astype(BF)

    keep = [m for m in range(tp_count) if m % CORES == 0]
    came = [over_tp(partials[m ^ 1], 1) for m in keep]
    sums = call(add, [out_piece] * len(keep), [partials[m] for m in keep] + came)
    kept = [sums[0], over_tp(sums[1], CORES)]

    def expert(*refs):
        mine_ref, came_ref, ws, outs = refs[0], refs[1], refs[2:8], refs[8:]
        total = [None, None]
        for wg, wu, wd in (ws[0:3], ws[3:6]):
            gate = dot(mine_ref[...], wg[at_half(False), :]) + dot(came_ref[...], wg[at_half(True), :])
            up = dot(mine_ref[...], wu[at_half(False), :]) + dot(came_ref[...], wu[at_half(True), :])
            hidden = swiglu(gate, up)
            for i in range(2):
                term = dot(hidden, wd[:, at_half(i == 1)])
                total[i] = term if total[i] is None else total[i] + term
        for i in range(2):
            outs[i][...] = total[i].astype(BF)

    returned = []
    for x, s in zip(arrived, order):
        came = over_tp(x, CORES)
        mine, other = call(expert, [piece] * 2, [x, came, w_gate, w_up, w_down, near_gate, near_up, near_down])
        more = over_tp(other, CORES)
        (out,) = call(add, [piece], [mine, more])
        returned.append(over_ep(out, ep_count - s))

    def combine(info_ref, *refs):
        chosen, back, sofar, outs = refs[:top], refs[top], refs[top + 1 : -2], refs[-2:]
        core = lax.axis_index("tp") % CORES
        for i in range(2):
            at = pl.ds(pl.multiple_of((core if i == 0 else 1 - core) * quarter, quarter), quarter)
            total = sofar[i][...].astype(F32) if sofar else jnp.zeros((rows, quarter), F32)
            for k in range(top):
                total = total + dot(chosen[k][...], back[:, at]) * info_ref[:, top + k : top + k + 1]
            outs[i][...] = total.astype(outs[i].dtype)

    sofar = []
    wide = jax.ShapeDtypeStruct((rows, quarter), F32)
    for i, (back, s) in enumerate(zip(returned, order)):
        kind = [wide, out_piece if i + 1 == len(order) else wide]
        sofar = call(combine, kind, [info, *picks[i * top : i * top + top], back, *sofar])

    def finish(mine_ref, more_ref, near_ref, far_ref, out_ref):
        total = mine_ref[...] + more_ref[...].astype(F32)
        out_ref[...] = (total + near_ref[...].astype(F32) + far_ref[...].astype(F32)).astype(BF)

    return call(finish, out_piece, [sofar[0], over_tp(sofar[1], 1), *kept])


CORES = 2


def shift_order(ep_count):
    return list(range(1, ep_count))


def general_body(
    tokens, norm_gain, routing, gate_weights, expert_gate, expert_up, expert_down, shared_gate, shared_up, shared_down
):
    ep_count = lax.axis_size("ep")
    tp_count = lax.axis_size("tp")
    tok_rows, width = tokens.shape
    top = routing.shape[1]
    local_experts = expert_gate.shape[0]
    experts = ep_count * local_experts
    capacity = max(2, 3 * tok_rows * top // (2 * experts))
    quarter = width // tp_count
    arrived_rows = ep_count * capacity
    normed = norm_rows(tokens, norm_gain)
    flat_experts = routing.reshape(-1)
    assign = flat_experts.shape[0]
    onehot = (flat_experts[:, None] == jnp.arange(experts, dtype=jnp.int32)[None, :]).astype(jnp.float32)
    lower = (jnp.arange(assign)[:, None] >= jnp.arange(assign)[None, :]).astype(jnp.float32)
    running = jnp.dot(lower, onehot, precision=lax.Precision.HIGHEST)
    slot = (jnp.sum(running * onehot, axis=1) - 1.0).astype(jnp.int32)
    dest = flat_experts * capacity + slot
    owner = jnp.arange(assign, dtype=jnp.int32) // top
    slot_token = jnp.full((experts * capacity,), tok_rows, jnp.int32).at[dest].set(owner)
    padded = jnp.concatenate([normed, jnp.zeros((1, width), jnp.bfloat16)], axis=0)
    outgoing = padded[slot_token].reshape(experts, capacity, width)
    position = lax.axis_index("tp")
    own_columns = lax.dynamic_slice_in_dim(outgoing, position * quarter, quarter, 2)
    arrived = lax.all_to_all(own_columns, "ep", split_axis=0, concat_axis=0, tiled=True)
    piece = lax.all_gather(arrived, "tp", axis=2, tiled=True)
    piece = piece.reshape(ep_count, local_experts, capacity, width)
    routed_list = []
    for local in range(local_experts):
        rows = piece[:, local].reshape(arrived_rows, width)
        gate = jnp.dot(rows, expert_gate[local], preferred_element_type=jnp.float32)
        up = jnp.dot(rows, expert_up[local], preferred_element_type=jnp.float32)
        hidden = (jax.nn.silu(gate) * up).astype(jnp.bfloat16)
        term = jnp.dot(hidden, expert_down[local], preferred_element_type=jnp.float32)
        routed_list.append(term.reshape(ep_count, capacity, width))
    routed_terms = jnp.stack(routed_list, axis=1).reshape(experts * capacity, width)
    shared_gate_rows = jnp.dot(normed, shared_gate, preferred_element_type=jnp.float32)
    shared_up_rows = jnp.dot(normed, shared_up, preferred_element_type=jnp.float32)
    shared_hidden = (jax.nn.silu(shared_gate_rows) * shared_up_rows).astype(jnp.bfloat16)
    shared_term = jnp.dot(shared_hidden, shared_down, preferred_element_type=jnp.float32)
    routed_sum, shared_sum = (
        lax.psum_scatter(x.astype(jnp.bfloat16), "tp", scatter_dimension=1, tiled=True).astype(jnp.float32)
        for x in (routed_terms, shared_term)
    )
    expert_out = routed_sum.astype(jnp.bfloat16).reshape(experts, capacity, quarter)
    returned = lax.all_to_all(expert_out, "ep", split_axis=0, concat_axis=0, tiled=True)
    picked = returned.reshape(experts * capacity, quarter)[dest]
    picked = picked.astype(jnp.float32).reshape(tok_rows, top, quarter)
    routed = jnp.sum(picked * gate_weights[:, :, None], axis=1)
    return (routed + shared_sum).astype(jnp.bfloat16)


def solution(mesh):
    in_specs = (
        P(("grp", "ep"), None),
        P(),
        P(("grp", "ep"), None),
        P(("grp", "ep"), None),
        P("ep", None, "tp"),
        P("ep", None, "tp"),
        P("ep", "tp", None),
        P(None, "tp"),
        P(None, "tp"),
        P("tp", None),
    )
    ep_count, tp_count = mesh.shape["ep"], mesh.shape["tp"]

    def step(body):
        return jax.shard_map(body, mesh=mesh, in_specs=in_specs, out_specs=P(("grp", "ep"), "tp"), check_vma=False)

    if ep_count <= 2 * tp_count and tp_count == 2 * CORES:
        return step(fast_body)
    return step(general_body)
```

```python
import jax
import jax.numpy as jnp
from jax import lax
from jax.experimental import pallas as pl
from jax.experimental.pallas import tpu as pltpu
from jax.sharding import PartitionSpec as P


BF, F32 = jnp.bfloat16, jnp.float32
VM = pltpu.MemorySpace.VMEM


def norm_rows(tokens, norm_gain):
    values = tokens.astype(jnp.float32)
    scale = lax.rsqrt(jnp.mean(values * values, axis=-1, keepdims=True) + 1e-06)
    return (values * scale * norm_gain).astype(jnp.bfloat16)


def dot(a, b):
    return jnp.dot(a, b, preferred_element_type=F32)


def swiglu(gate, up):
    return (gate / (1.0 + jnp.exp(-gate)) * up).astype(BF)


def call(kernel, outs, args, loads=0, mib=16, **more):
    return pl.pallas_call(
        kernel,
        out_shape=outs,
        in_specs=[pl.BlockSpec(memory_space=VM)] * (len(args) - loads)
        + [pl.BlockSpec(memory_space=pltpu.MemorySpace.HBM)] * loads,
        out_specs=jax.tree.map(lambda _: pl.BlockSpec(memory_space=VM), outs),
        compiler_params=pltpu.CompilerParams(vmem_limit_bytes=mib * 1024 * 1024),
        **more,
    )(*args)


def places_of(routing, ep, experts, capacity):
    top, rows = routing.shape
    expert = lax.broadcasted_iota(jnp.int32, (max(8, experts), rows), 0)
    hits = [(routing[k : k + 1, :] == expert).astype(F32) for k in range(top)]
    named = sum(hits[1:], hits[0])
    before = lax.broadcasted_iota(jnp.int32, (rows, rows), 0)
    at = lax.broadcasted_iota(jnp.int32, (rows, rows), 1)
    earlier = dot(named.astype(BF), (before < at).astype(F32).astype(BF))
    places = []
    for k in range(top):
        slot = jnp.sum(earlier * hits[k], axis=0, keepdims=True)
        turn = routing[k : k + 1, :] - ep
        turn = jnp.where(turn < 0, turn + experts, turn)
        places.append((turn * capacity).astype(F32) + slot)
    return places


def fast_body(
    tokens, norm_gain, routing, gate_weights, expert_gate, expert_up, expert_down, shared_gate, shared_up, shared_down
):
    ep_count, tp_count = lax.axis_size("ep"), lax.axis_size("tp")
    rows, width = tokens.shape
    top = routing.shape[1]
    experts = ep_count
    capacity = max(2, 3 * rows * top // (2 * experts))
    quarter = width // tp_count
    half = width // 2
    part = capacity // CORES
    w_gate, w_up, w_down = expert_gate[0], expert_up[0], expert_down[0]
    order = shift_order(ep_count)
    routing, gate_weights = routing.T, gate_weights.T

    def over_tp(x, m):
        return lax.ppermute(x, "tp", [(i, i ^ m) for i in range(tp_count)])

    def over_ep(x, s):
        return lax.ppermute(x, "ep", [(i, (i + s) % ep_count) for i in range(ep_count)])

    def at_quarter(m):
        return pl.ds(pl.multiple_of((lax.axis_index("tp") ^ m) * quarter, quarter), quarter)

    def at_half(other):
        chip = lax.axis_index("tp") // CORES
        return pl.ds(pl.multiple_of((1 - chip if other else chip) * half, half), half)

    near_gate, near_up = over_tp(w_gate, 1), over_tp(w_up, 1)
    near_down = over_tp(w_down, 1)

    blocks = 4
    step = rows // blocks

    def dispatch(tokens_hbm, gain_hbm, routing_hbm, normed_ref, *refs):
        send_refs, (tokens_ref, gain_ref, routing_ref, sems) = refs[: len(order)], refs[len(order) :]
        chunks = [pl.ds(i * step, step) for i in range(blocks)]
        loads = [(routing_hbm, routing_ref), (gain_hbm, gain_ref)]
        loads += [(tokens_hbm.at[c], tokens_ref.at[c]) for c in chunks]
        copies = [pltpu.make_async_copy(src, dst, sems.at[i]) for i, (src, dst) in enumerate(loads)]
        for copy in copies:
            copy.start()
        copies[0].wait()
        places = places_of(routing_ref[...], lax.axis_index("ep"), experts, capacity)
        places = [p.astype(jnp.int32) for p in places]
        copies[1].wait()
        for c, copy in zip(chunks, copies[2:]):
            copy.wait()
            values = tokens_ref[c, :].astype(F32)
            scale = lax.rsqrt(jnp.mean(values * values, axis=-1, keepdims=True) + 1e-06)
            normed_ref[c, :] = (values * scale * gain_ref[...]).astype(BF)
        mine = normed_ref[:, at_half(False)]
        base = (lax.axis_index("tp") % CORES) * part
        for send_ref, s in zip(send_refs, order):
            index = lax.broadcasted_iota(jnp.int32, (part, rows), 0) + (base + s * capacity)
            pick = (index == places[0]).astype(F32)
            for p in places[1:]:
                pick = pick + (index == p).astype(F32)
            send_ref[...] = dot(pick.astype(BF), mine).astype(BF)

    piece = jax.ShapeDtypeStruct((part, half), BF)
    normed, *sends = call(
        dispatch,
        [jax.ShapeDtypeStruct((rows, width), BF)] + [piece] * len(order),
        [tokens, norm_gain.reshape(1, width), routing],
        loads=3,
        scratch_shapes=[
            pltpu.VMEM((rows, width), BF),
            pltpu.VMEM((1, width), F32),
            pltpu.VMEM((top, rows), jnp.int32),
            pltpu.SemaphoreType.DMA((blocks + 2,)),
        ],
    )
    arrived = [over_ep(x, s) for x, s in zip(sends, order)]

    stored = [routing, gate_weights, w_gate, w_up, shared_gate, shared_up, w_down, shared_down]

    def local(normed_ref, *refs):
        sources, refs = refs[: len(stored)], refs[len(stored) :]
        out_refs, info_ref, refs = refs[:tp_count], refs[tp_count], refs[tp_count + 1 :]
        pick_refs, targets, sems = refs[: -len(stored) - 1], refs[-len(stored) - 1 : -1], refs[-1]
        copies = [pltpu.make_async_copy(a, b, sems.at[i]) for i, (a, b) in enumerate(zip(sources, targets))]
        for copy in copies:
            copy.start()
        routing_ref, gw_ref, wg, wu, sg, su, wd, sd = targets
        copies[0].wait()
        copies[1].wait()
        places = places_of(routing_ref[...], lax.axis_index("ep"), experts, capacity)
        index = lax.broadcasted_iota(jnp.int32, (capacity, rows), 0)
        own = (index == places[0].astype(jnp.int32)).astype(F32)
        for p in places[1:]:
            own = own + (index == p.astype(jnp.int32)).astype(F32)
        own_rows = dot(own.astype(BF), normed_ref[...]).astype(BF)
        copies[2].wait()
        copies[3].wait()
        hidden = swiglu(dot(own_rows, wg[...]), dot(own_rows, wu[...]))
        copies[4].wait()
        copies[5].wait()
        s_hidden = swiglu(dot(normed_ref[...], sg[...]), dot(normed_ref[...], su[...]))
        info = jnp.zeros((128, rows), F32)
        line = lax.broadcasted_iota(jnp.int32, (128, rows), 0)
        for k in range(top):
            info = jnp.where(line == k, places[k], info)
            info = jnp.where(line == top + k, gw_ref[k : k + 1, :], info)
        info = info.T
        info_ref[...] = info
        lanes = lax.broadcasted_iota(jnp.int32, (rows, capacity), 1)
        columns = [info[:, k : k + 1].astype(jnp.int32) for k in range(top)]
        weights = [info[:, top + k : top + k + 1] for k in range(top)]
        pick = (columns[0] == lanes).astype(F32)
        weight = jnp.where(columns[0] < capacity, weights[0], 0.0)
        for k in range(1, top):
            pick = pick + (columns[k] == lanes).astype(F32)
            weight = weight + jnp.where(columns[k] < capacity, weights[k], 0.0)
        pick = pick.astype(BF)
        copies[6].wait()
        copies[7].wait()
        for m in range(tp_count):
            term = dot(hidden, wd[:, at_quarter(m)]).astype(BF)
            shared = dot(s_hidden, sd[:, at_quarter(m)])
            out_refs[m][...] = (dot(pick, term) * weight + shared).astype(BF)
        lanes = lax.broadcasted_iota(jnp.int32, (rows, part), 1)
        base = (lax.axis_index("tp") % CORES) * part
        for i, s in enumerate(order):
            for k in range(top):
                pick_refs[i * top + k][...] = (columns[k] == lanes + (base + s * capacity)).astype(F32).astype(BF)

    out_piece = jax.ShapeDtypeStruct((rows, quarter), BF)
    partials = call(
        local,
        [out_piece] * tp_count
        + [jax.ShapeDtypeStruct((rows, 128), F32)]
        + [jax.ShapeDtypeStruct((rows, part), BF)] * (top * len(order)),
        [normed, *stored],
        loads=len(stored),
        scratch_shapes=[pltpu.VMEM(x.shape, x.dtype) for x in stored] + [pltpu.SemaphoreType.DMA((len(stored),))],
    )
    info, picks = partials[tp_count], partials[tp_count + 1 :]
    partials = partials[:tp_count]

    def add(*refs):
        n = len(refs) // 3
        for i in range(n):
            refs[2 * n + i][...] = (refs[i][...].astype(F32) + refs[n + i][...].astype(F32)).astype(BF)

    keep = [m for m in range(tp_count) if m % CORES == 0]
    came = [over_tp(partials[m ^ 1], 1) for m in keep]
    sums = call(add, [out_piece] * len(keep), [partials[m] for m in keep] + came)
    kept = [sums[0], over_tp(sums[1], CORES)]

    def expert(*refs):
        mine_ref, came_ref, ws, outs = refs[0], refs[1], refs[2:8], refs[8:]
        total = [None, None]
        for wg, wu, wd in (ws[0:3], ws[3:6]):
            gate = dot(mine_ref[...], wg[at_half(False), :]) + dot(came_ref[...], wg[at_half(True), :])
            up = dot(mine_ref[...], wu[at_half(False), :]) + dot(came_ref[...], wu[at_half(True), :])
            hidden = swiglu(gate, up)
            for i in range(2):
                term = dot(hidden, wd[:, at_half(i == 1)])
                total[i] = term if total[i] is None else total[i] + term
        for i in range(2):
            outs[i][...] = total[i].astype(BF)

    returned = []
    for x, s in zip(arrived, order):
        came = over_tp(x, CORES)
        mine, other = call(expert, [piece] * 2, [x, came, w_gate, w_up, w_down, near_gate, near_up, near_down])
        more = over_tp(other, CORES)
        (out,) = call(add, [piece], [mine, more])
        returned.append(over_ep(out, ep_count - s))

    def combine(info_ref, *refs):
        chosen, back, sofar, outs = refs[:top], refs[top], refs[top + 1 : -2], refs[-2:]
        core = lax.axis_index("tp") % CORES
        for i in range(2):
            at = pl.ds(pl.multiple_of((core if i == 0 else 1 - core) * quarter, quarter), quarter)
            total = sofar[i][...].astype(F32) if sofar else jnp.zeros((rows, quarter), F32)
            for k in range(top):
                total = total + dot(chosen[k][...], back[:, at]) * info_ref[:, top + k : top + k + 1]
            outs[i][...] = total.astype(outs[i].dtype)

    sofar = []
    wide = jax.ShapeDtypeStruct((rows, quarter), F32)
    for i, (back, s) in enumerate(zip(returned, order)):
        kind = [wide, out_piece if i + 1 == len(order) else wide]
        sofar = call(combine, kind, [info, *picks[i * top : i * top + top], back, *sofar])

    def finish(mine_ref, more_ref, near_ref, far_ref, out_ref):
        total = mine_ref[...] + more_ref[...].astype(F32)
        out_ref[...] = (total + near_ref[...].astype(F32) + far_ref[...].astype(F32)).astype(BF)

    return call(finish, out_piece, [sofar[0], over_tp(sofar[1], 1), *kept])


CORES = 2


def shift_order(ep_count):
    return list(range(1, ep_count))


def general_body(
    tokens, norm_gain, routing, gate_weights, expert_gate, expert_up, expert_down, shared_gate, shared_up, shared_down
):
    ep_count = lax.axis_size("ep")
    tp_count = lax.axis_size("tp")
    tok_rows, width = tokens.shape
    top = routing.shape[1]
    local_experts = expert_gate.shape[0]
    experts = ep_count * local_experts
    capacity = max(2, 3 * tok_rows * top // (2 * experts))
    quarter = width // tp_count
    arrived_rows = ep_count * capacity
    normed = norm_rows(tokens, norm_gain)
    flat_experts = routing.reshape(-1)
    assign = flat_experts.shape[0]
    onehot = (flat_experts[:, None] == jnp.arange(experts, dtype=jnp.int32)[None, :]).astype(jnp.float32)
    lower = (jnp.arange(assign)[:, None] >= jnp.arange(assign)[None, :]).astype(jnp.float32)
    running = jnp.dot(lower, onehot, precision=lax.Precision.HIGHEST)
    slot = (jnp.sum(running * onehot, axis=1) - 1.0).astype(jnp.int32)
    dest = flat_experts * capacity + slot
    owner = jnp.arange(assign, dtype=jnp.int32) // top
    slot_token = jnp.full((experts * capacity,), tok_rows, jnp.int32).at[dest].set(owner)
    padded = jnp.concatenate([normed, jnp.zeros((1, width), jnp.bfloat16)], axis=0)
    outgoing = padded[slot_token].reshape(experts, capacity, width)
    position = lax.axis_index("tp")
    own_columns = lax.dynamic_slice_in_dim(outgoing, position * quarter, quarter, 2)
    arrived = lax.all_to_all(own_columns, "ep", split_axis=0, concat_axis=0, tiled=True)
    piece = lax.all_gather(arrived, "tp", axis=2, tiled=True)
    piece = piece.reshape(ep_count, local_experts, capacity, width)
    routed_list = []
    for local in range(local_experts):
        rows = piece[:, local].reshape(arrived_rows, width)
        gate = jnp.dot(rows, expert_gate[local], preferred_element_type=jnp.float32)
        up = jnp.dot(rows, expert_up[local], preferred_element_type=jnp.float32)
        hidden = (jax.nn.silu(gate) * up).astype(jnp.bfloat16)
        term = jnp.dot(hidden, expert_down[local], preferred_element_type=jnp.float32)
        routed_list.append(term.reshape(ep_count, capacity, width))
    routed_terms = jnp.stack(routed_list, axis=1).reshape(experts * capacity, width)
    shared_gate_rows = jnp.dot(normed, shared_gate, preferred_element_type=jnp.float32)
    shared_up_rows = jnp.dot(normed, shared_up, preferred_element_type=jnp.float32)
    shared_hidden = (jax.nn.silu(shared_gate_rows) * shared_up_rows).astype(jnp.bfloat16)
    shared_term = jnp.dot(shared_hidden, shared_down, preferred_element_type=jnp.float32)
    routed_sum, shared_sum = (
        lax.psum_scatter(x.astype(jnp.bfloat16), "tp", scatter_dimension=1, tiled=True).astype(jnp.float32)
        for x in (routed_terms, shared_term)
    )
    expert_out = routed_sum.astype(jnp.bfloat16).reshape(experts, capacity, quarter)
    returned = lax.all_to_all(expert_out, "ep", split_axis=0, concat_axis=0, tiled=True)
    picked = returned.reshape(experts * capacity, quarter)[dest]
    picked = picked.astype(jnp.float32).reshape(tok_rows, top, quarter)
    routed = jnp.sum(picked * gate_weights[:, :, None], axis=1)
    return (routed + shared_sum).astype(jnp.bfloat16)


def solution(mesh):
    in_specs = (
        P(("grp", "ep"), None),
        P(),
        P(("grp", "ep"), None),
        P(("grp", "ep"), None),
        P("ep", None, "tp"),
        P("ep", None, "tp"),
        P("ep", "tp", None),
        P(None, "tp"),
        P(None, "tp"),
        P("tp", None),
    )
    ep_count, tp_count = mesh.shape["ep"], mesh.shape["tp"]

    def step(body):
        return jax.shard_map(body, mesh=mesh, in_specs=in_specs, out_specs=P(("grp", "ep"), "tp"), check_vma=False)

    if ep_count <= 2 * tp_count and tp_count == 2 * CORES:
        return step(fast_body)
    return step(general_body)
```

```python
import jax
import jax.numpy as jnp
from jax import lax
from jax.experimental import pallas as pl
from jax.experimental.pallas import tpu as pltpu
from jax.sharding import PartitionSpec as P


BF, F32 = jnp.bfloat16, jnp.float32
VM = pltpu.MemorySpace.VMEM


def norm_rows(tokens, norm_gain):
    values = tokens.astype(jnp.float32)
    scale = lax.rsqrt(jnp.mean(values * values, axis=-1, keepdims=True) + 1e-06)
    return (values * scale * norm_gain).astype(jnp.bfloat16)


def dot(a, b):
    return jnp.dot(a, b, preferred_element_type=F32)


def swiglu(gate, up):
    return (gate / (1.0 + jnp.exp(-gate)) * up).astype(BF)


def call(kernel, outs, args, loads=0, mib=16, **more):
    first = len(args) - loads
    args = [pltpu.with_memory_space_constraint(x, pltpu.HBM) if i >= first else x for i, x in enumerate(args)]
    return pl.pallas_call(
        kernel,
        out_shape=outs,
        in_specs=[pl.BlockSpec(memory_space=VM)] * (len(args) - loads)
        + [pl.BlockSpec(memory_space=pltpu.MemorySpace.HBM)] * loads,
        out_specs=jax.tree.map(lambda _: pl.BlockSpec(memory_space=VM), outs),
        compiler_params=pltpu.CompilerParams(vmem_limit_bytes=mib * 1024 * 1024),
        **more,
    )(*args)


def places_of(routing, ep, experts, capacity):
    top, rows = routing.shape
    expert = lax.broadcasted_iota(jnp.int32, (max(8, experts), rows), 0)
    hits = [(routing[k : k + 1, :] == expert).astype(F32) for k in range(top)]
    named = sum(hits[1:], hits[0])
    before = lax.broadcasted_iota(jnp.int32, (rows, rows), 0)
    at = lax.broadcasted_iota(jnp.int32, (rows, rows), 1)
    earlier = dot(named.astype(BF), (before < at).astype(F32).astype(BF))
    places = []
    for k in range(top):
        slot = jnp.sum(earlier * hits[k], axis=0, keepdims=True)
        turn = routing[k : k + 1, :] - ep
        turn = jnp.where(turn < 0, turn + experts, turn)
        places.append((turn * capacity).astype(F32) + slot)
    return places


def fast_body(
    tokens, norm_gain, routing, gate_weights, expert_gate, expert_up, expert_down, shared_gate, shared_up, shared_down
):
    ep_count, tp_count = lax.axis_size("ep"), lax.axis_size("tp")
    rows, width = tokens.shape
    top = routing.shape[1]
    experts = ep_count
    capacity = max(2, 3 * rows * top // (2 * experts))
    quarter = width // tp_count
    half = width // 2
    part = capacity // CORES
    hid = expert_gate.shape[2]
    w_gate, w_up, w_down = expert_gate[0], expert_up[0], expert_down[0]
    order = shift_order(ep_count)
    routing, gate_weights = routing.T, gate_weights.T

    def over_tp(x, m):
        return lax.ppermute(x, "tp", [(i, i ^ m) for i in range(tp_count)])

    def over_ep(x, s):
        return lax.ppermute(x, "ep", [(i, (i + s) % ep_count) for i in range(ep_count)])

    def at_quarter(m):
        return pl.ds(pl.multiple_of((lax.axis_index("tp") ^ m) * quarter, quarter), quarter)

    def at_half(other):
        chip = lax.axis_index("tp") // CORES
        return pl.ds(pl.multiple_of((1 - chip if other else chip) * half, half), half)

    near_gate, near_up = over_tp(w_gate, 1), over_tp(w_up, 1)
    near_down = over_tp(w_down, 1)

    blocks = 4
    step = rows // blocks

    def dispatch(tokens_hbm, gain_hbm, routing_hbm, down_hbm, normed_ref, far_ref, *refs):
        send_refs, (tokens_ref, gain_ref, routing_ref, sems) = refs[: len(order)], refs[len(order) :]
        chunks = [pl.ds(i * step, step) for i in range(blocks)]
        loads = [(routing_hbm, routing_ref), (gain_hbm, gain_ref)]
        loads += [(tokens_hbm.at[c], tokens_ref.at[c]) for c in chunks]
        loads += [(down_hbm.at[:, at_half(True)], far_ref)]
        copies = [pltpu.make_async_copy(src, dst, sems.at[i]) for i, (src, dst) in enumerate(loads)]
        for copy in copies:
            copy.start()
        copies[0].wait()
        places = places_of(routing_ref[...], lax.axis_index("ep"), experts, capacity)
        places = [p.astype(jnp.int32) for p in places]
        copies[1].wait()
        for c, copy in zip(chunks, copies[2:-1]):
            copy.wait()
            values = tokens_ref[c, :].astype(F32)
            scale = lax.rsqrt(jnp.mean(values * values, axis=-1, keepdims=True) + 1e-06)
            normed_ref[c, :] = (values * scale * gain_ref[...]).astype(BF)
        mine = normed_ref[:, at_half(False)]
        base = (lax.axis_index("tp") % CORES) * part
        for send_ref, s in zip(send_refs, order):
            index = lax.broadcasted_iota(jnp.int32, (part, rows), 0) + (base + s * capacity)
            pick = (index == places[0]).astype(F32)
            for p in places[1:]:
                pick = pick + (index == p).astype(F32)
            send_ref[...] = dot(pick.astype(BF), mine).astype(BF)
        copies[-1].wait()

    piece = jax.ShapeDtypeStruct((part, half), BF)
    normed, far_half, *sends = call(
        dispatch,
        [jax.ShapeDtypeStruct((rows, width), BF), jax.ShapeDtypeStruct((hid, half), BF)] + [piece] * len(order),
        [tokens, norm_gain.reshape(1, width), routing, w_down],
        loads=4,
        scratch_shapes=[
            pltpu.VMEM((rows, width), BF),
            pltpu.VMEM((1, width), F32),
            pltpu.VMEM((top, rows), jnp.int32),
            pltpu.SemaphoreType.DMA((blocks + 3,)),
        ],
    )
    far_down = over_tp(far_half, CORES)
    last_down = over_tp(far_down, 1)
    arrived = [over_ep(x, s) for x, s in zip(sends, order)]

    stored = [routing, gate_weights, w_gate, w_up, shared_gate, shared_up, w_down, shared_down]

    def local(normed_ref, *refs):
        sources, refs = refs[: len(stored)], refs[len(stored) :]
        out_refs, info_ref, refs = refs[:tp_count], refs[tp_count], refs[tp_count + 1 :]
        pick_refs, targets, sems = refs[: -len(stored) - 1], refs[-len(stored) - 1 : -1], refs[-1]
        copies = [pltpu.make_async_copy(a, b, sems.at[i]) for i, (a, b) in enumerate(zip(sources, targets))]
        for copy in copies:
            copy.start()
        routing_ref, gw_ref, wg, wu, sg, su, wd, sd = targets
        copies[0].wait()
        copies[1].wait()
        places = places_of(routing_ref[...], lax.axis_index("ep"), experts, capacity)
        index = lax.broadcasted_iota(jnp.int32, (capacity, rows), 0)
        own = (index == places[0].astype(jnp.int32)).astype(F32)
        for p in places[1:]:
            own = own + (index == p.astype(jnp.int32)).astype(F32)
        own_rows = dot(own.astype(BF), normed_ref[...]).astype(BF)
        copies[2].wait()
        copies[3].wait()
        hidden = swiglu(dot(own_rows, wg[...]), dot(own_rows, wu[...]))
        copies[4].wait()
        copies[5].wait()
        s_hidden = swiglu(dot(normed_ref[...], sg[...]), dot(normed_ref[...], su[...]))
        info = jnp.zeros((128, rows), F32)
        line = lax.broadcasted_iota(jnp.int32, (128, rows), 0)
        for k in range(top):
            info = jnp.where(line == k, places[k], info)
            info = jnp.where(line == top + k, gw_ref[k : k + 1, :], info)
        info = info.T
        info_ref[...] = info
        lanes = lax.broadcasted_iota(jnp.int32, (rows, capacity), 1)
        columns = [info[:, k : k + 1].astype(jnp.int32) for k in range(top)]
        weights = [info[:, top + k : top + k + 1] for k in range(top)]
        pick = (columns[0] == lanes).astype(F32)
        weight = jnp.where(columns[0] < capacity, weights[0], 0.0)
        for k in range(1, top):
            pick = pick + (columns[k] == lanes).astype(F32)
            weight = weight + jnp.where(columns[k] < capacity, weights[k], 0.0)
        pick = pick.astype(BF)
        copies[6].wait()
        copies[7].wait()
        for m in range(tp_count):
            term = dot(hidden, wd[:, at_quarter(m)]).astype(BF)
            shared = dot(s_hidden, sd[:, at_quarter(m)])
            out_refs[m][...] = (dot(pick, term) * weight + shared).astype(BF)
        lanes = lax.broadcasted_iota(jnp.int32, (rows, part), 1)
        base = (lax.axis_index("tp") % CORES) * part
        for i, s in enumerate(order):
            for k in range(top):
                pick_refs[i * top + k][...] = (columns[k] == lanes + (base + s * capacity)).astype(F32).astype(BF)

    out_piece = jax.ShapeDtypeStruct((rows, quarter), BF)
    partials = call(
        local,
        [out_piece] * tp_count
        + [jax.ShapeDtypeStruct((rows, 128), F32)]
        + [jax.ShapeDtypeStruct((rows, part), BF)] * (top * len(order)),
        [normed, *stored],
        loads=len(stored),
        scratch_shapes=[pltpu.VMEM(x.shape, x.dtype) for x in stored] + [pltpu.SemaphoreType.DMA((len(stored),))],
    )
    info, picks = partials[tp_count], partials[tp_count + 1 :]
    partials = partials[:tp_count]

    def add(*refs):
        n = len(refs) // 3
        for i in range(n):
            refs[2 * n + i][...] = (refs[i][...].astype(F32) + refs[n + i][...].astype(F32)).astype(BF)

    keep = [m for m in range(tp_count) if m % CORES == 0]
    came = [over_tp(partials[m ^ 1], 1) for m in keep]
    sums = call(add, [out_piece] * len(keep), [partials[m] for m in keep] + came)
    kept = [sums[0], over_tp(sums[1], CORES)]

    def first(mine_ref, came_ref, *refs):
        ws, out_ref = refs[:4], refs[4]
        for i, (wg, wu) in enumerate((ws[:2], ws[2:])):
            gate = dot(mine_ref[...], wg[at_half(False), :]) + dot(came_ref[...], wg[at_half(True), :])
            up = dot(mine_ref[...], wu[at_half(False), :]) + dot(came_ref[...], wu[at_half(True), :])
            out_ref[:, i * hid : (i + 1) * hid] = swiglu(gate, up)

    def second(mine_ref, came_ref, own_ref, near_ref, far_ref, last_ref, out_ref):
        total = dot(mine_ref[:, :hid], own_ref[:, at_half(False)]) + dot(mine_ref[:, hid:], near_ref[:, at_half(False)])
        total = total + dot(came_ref[:, :hid], far_ref[...]) + dot(came_ref[:, hid:], last_ref[...])
        out_ref[...] = total.astype(BF)

    returned = []
    for x, s in zip(arrived, order):
        came = over_tp(x, CORES)
        hidden = call(first, jax.ShapeDtypeStruct((part, CORES * hid), BF), [x, came, w_gate, w_up, near_gate, near_up])
        more = over_tp(hidden, CORES)
        out = call(second, piece, [hidden, more, w_down, near_down, far_down, last_down])
        returned.append(over_ep(out, ep_count - s))

    def combine(info_ref, *refs):
        chosen, back, sofar, outs = refs[:top], refs[top], refs[top + 1 : -2], refs[-2:]
        core = lax.axis_index("tp") % CORES
        for i in range(2):
            at = pl.ds(pl.multiple_of((core if i == 0 else 1 - core) * quarter, quarter), quarter)
            total = sofar[i][...].astype(F32) if sofar else jnp.zeros((rows, quarter), F32)
            for k in range(top):
                total = total + dot(chosen[k][...], back[:, at]) * info_ref[:, top + k : top + k + 1]
            outs[i][...] = total.astype(outs[i].dtype)

    sofar = []
    wide = jax.ShapeDtypeStruct((rows, quarter), F32)
    for i, (back, s) in enumerate(zip(returned, order)):
        kind = [wide, out_piece if i + 1 == len(order) else wide]
        sofar = call(combine, kind, [info, *picks[i * top : i * top + top], back, *sofar])

    def finish(mine_ref, more_ref, near_ref, far_ref, out_ref):
        total = mine_ref[...] + more_ref[...].astype(F32)
        out_ref[...] = (total + near_ref[...].astype(F32) + far_ref[...].astype(F32)).astype(BF)

    return call(finish, out_piece, [sofar[0], over_tp(sofar[1], 1), *kept])


CORES = 2


def shift_order(ep_count):
    return list(range(1, ep_count))


def general_body(
    tokens, norm_gain, routing, gate_weights, expert_gate, expert_up, expert_down, shared_gate, shared_up, shared_down
):
    ep_count = lax.axis_size("ep")
    tp_count = lax.axis_size("tp")
    tok_rows, width = tokens.shape
    top = routing.shape[1]
    local_experts = expert_gate.shape[0]
    experts = ep_count * local_experts
    capacity = max(2, 3 * tok_rows * top // (2 * experts))
    quarter = width // tp_count
    arrived_rows = ep_count * capacity
    normed = norm_rows(tokens, norm_gain)
    flat_experts = routing.reshape(-1)
    assign = flat_experts.shape[0]
    onehot = (flat_experts[:, None] == jnp.arange(experts, dtype=jnp.int32)[None, :]).astype(jnp.float32)
    lower = (jnp.arange(assign)[:, None] >= jnp.arange(assign)[None, :]).astype(jnp.float32)
    running = jnp.dot(lower, onehot, precision=lax.Precision.HIGHEST)
    slot = (jnp.sum(running * onehot, axis=1) - 1.0).astype(jnp.int32)
    dest = flat_experts * capacity + slot
    owner = jnp.arange(assign, dtype=jnp.int32) // top
    slot_token = jnp.full((experts * capacity,), tok_rows, jnp.int32).at[dest].set(owner)
    padded = jnp.concatenate([normed, jnp.zeros((1, width), jnp.bfloat16)], axis=0)
    outgoing = padded[slot_token].reshape(experts, capacity, width)
    position = lax.axis_index("tp")
    own_columns = lax.dynamic_slice_in_dim(outgoing, position * quarter, quarter, 2)
    arrived = lax.all_to_all(own_columns, "ep", split_axis=0, concat_axis=0, tiled=True)
    piece = lax.all_gather(arrived, "tp", axis=2, tiled=True)
    piece = piece.reshape(ep_count, local_experts, capacity, width)
    routed_list = []
    for local in range(local_experts):
        rows = piece[:, local].reshape(arrived_rows, width)
        gate = jnp.dot(rows, expert_gate[local], preferred_element_type=jnp.float32)
        up = jnp.dot(rows, expert_up[local], preferred_element_type=jnp.float32)
        hidden = (jax.nn.silu(gate) * up).astype(jnp.bfloat16)
        term = jnp.dot(hidden, expert_down[local], preferred_element_type=jnp.float32)
        routed_list.append(term.reshape(ep_count, capacity, width))
    routed_terms = jnp.stack(routed_list, axis=1).reshape(experts * capacity, width)
    shared_gate_rows = jnp.dot(normed, shared_gate, preferred_element_type=jnp.float32)
    shared_up_rows = jnp.dot(normed, shared_up, preferred_element_type=jnp.float32)
    shared_hidden = (jax.nn.silu(shared_gate_rows) * shared_up_rows).astype(jnp.bfloat16)
    shared_term = jnp.dot(shared_hidden, shared_down, preferred_element_type=jnp.float32)
    routed_sum, shared_sum = (
        lax.psum_scatter(x.astype(jnp.bfloat16), "tp", scatter_dimension=1, tiled=True).astype(jnp.float32)
        for x in (routed_terms, shared_term)
    )
    expert_out = routed_sum.astype(jnp.bfloat16).reshape(experts, capacity, quarter)
    returned = lax.all_to_all(expert_out, "ep", split_axis=0, concat_axis=0, tiled=True)
    picked = returned.reshape(experts * capacity, quarter)[dest]
    picked = picked.astype(jnp.float32).reshape(tok_rows, top, quarter)
    routed = jnp.sum(picked * gate_weights[:, :, None], axis=1)
    return (routed + shared_sum).astype(jnp.bfloat16)


def solution(mesh):
    in_specs = (
        P(("grp", "ep"), None),
        P(),
        P(("grp", "ep"), None),
        P(("grp", "ep"), None),
        P("ep", None, "tp"),
        P("ep", None, "tp"),
        P("ep", "tp", None),
        P(None, "tp"),
        P(None, "tp"),
        P("tp", None),
    )
    ep_count, tp_count = mesh.shape["ep"], mesh.shape["tp"]

    def step(body):
        return jax.shard_map(body, mesh=mesh, in_specs=in_specs, out_specs=P(("grp", "ep"), "tp"), check_vma=False)

    if ep_count <= 2 * tp_count and tp_count == 2 * CORES:
        return step(fast_body)
    return step(general_body)
```
